32 devices in a mesh: sp: 8 (over z, core), tp: 4 (over y, x).
Axes of the slice: x: 2, y: 2, z: 4, core: 2. Of those that a mesh axis runs over, the one named last changes fastest.
Arguments:
- moe_input: bfloat16 [2048, 2048], P('sp', 'tp'), may hold values from -6 to 6
- out_grad: bfloat16 [2048, 2048], P('sp', 'tp'), may hold values from -8 to 8
- routes: int32 [2048, 2], P('sp'), may hold values from 0 to 7, all different within a row; in each aligned block of 256 rows (0 to 255, 256 to 511, ...) at most 80 rows name the same one
- route_weight: float32 [2048, 2], P('sp'), may hold values from 0.2 to 1.5
- w_gate: bfloat16 [8, 2048, 2048], P('sp', None, 'tp'), may hold values from -0.125 to 0.125
- w_up: bfloat16 [8, 2048, 2048], P('sp', None, 'tp'), may hold values from -0.125 to 0.125
- w_down: bfloat16 [8, 2048, 2048], P('sp', 'tp'), may hold values from -0.125 to 0.125
- w_out: bfloat16 [2048, 2048], P(None, 'tp'), may hold values from -0.125 to 0.125
- queries: bfloat16 [2048, 1024], P('sp', 'tp'), may hold values from -6 to 6
- key_rows: bfloat16 [2048, 1024], P('sp', 'tp'), may hold values from -6 to 6
- value_rows: bfloat16 [2048, 2048], P('sp', 'tp'), may hold values from -6 to 6
- log_decay: float32 [2048, 1024], P('sp', 'tp'), may hold values from -1 to 0
Outputs:
- grad_gate: bfloat16 [8, 2048, 2048], P('sp', None, 'tp')
- grad_up: bfloat16 [8, 2048, 2048], P('sp', None, 'tp')
- grad_down: bfloat16 [8, 2048, 2048], P('sp', 'tp')
- grad_proj: float32 [2048, 2048], P('sp', 'tp')
- grad_queries: bfloat16 [2048, 1024], P('sp', 'tp')
- grad_keys: bfloat16 [2048, 1024], P('sp', 'tp')
- grad_values: bfloat16 [2048, 2048], P('sp', 'tp')
- grad_decay: float32 [2048, 1024], P('sp', 'tp')
The draws below stay inside these ranges and needn't reach their ends.
Inputs may be any that keep to these rules, and one draw needn't show every extreme that they name: `routes`: A token's experts differ. Within each aligned block of 256 tokens no expert is named more than 80 times, and in some block one expert is named exactly 80 times.
All inputs are finite; a program needn't handle non-finite values.
Results may differ from the reference program's by a relative error of at most 0.025.
Values may be sent and summed in bfloat16 or wider, within the bound.
A program may use at most 64 MiB of HBM per device.

```python
import math
import jax
import jax.numpy as jnp
import numpy as np
from jax import lax

D = 2048
HEAD_COUNT = 32
KEY_CHANNELS = 32
VAL_DIM = 64
EXP_HIDDEN = 2048
TOP = 2
BLOCK = 64
TOK_DEV = 256
TOKEN_COUNT = 2048
EXPERTS = 8
CAP = 80
HID_DEV = 512
N_SP = 8
N_TP = 4


def draw_log_decay(key, part):
    sequence_lanes = jax.random.split(jax.random.fold_in(key, 17), 5)
    lagging_head = jax.random.uniform(sequence_lanes[0], (HEAD_COUNT,), jnp.float32) < 0.5
    base_rate = jnp.where(lagging_head, 0.5 / TOKEN_COUNT, 1.0 / 40.0)
    spans = TOKEN_COUNT // TOK_DEV
    span_scale = jnp.exp(jax.random.uniform(sequence_lanes[1], (spans,), jnp.float32, -0.7, 0.7))
    position_scale = jnp.repeat(span_scale, TOK_DEV)
    wobble = jnp.exp(jax.random.uniform(sequence_lanes[2], (TOKEN_COUNT, HEAD_COUNT, KEY_CHANNELS), jnp.float32, -1.0, 1.0))
    smoothed_decay = -(position_scale[:, None, None] * base_rate[None, :, None] * wobble)
    spike_position = jax.random.randint(sequence_lanes[3], (2,), 0, TOKEN_COUNT)
    spike_length = jnp.log(jax.random.uniform(sequence_lanes[4], (2,), jnp.float32, 0.5, 0.8))
    spike_rows = jnp.sum(jnp.where(jnp.arange(TOKEN_COUNT)[:, None] == spike_position[None, :], spike_length[None, :], 0.0), axis=1)
    spike_addend = spike_rows[:, None, None] * lagging_head[None, :, None].astype(jnp.float32)
    return (smoothed_decay + spike_addend).reshape(TOKEN_COUNT, HEAD_COUNT * KEY_CHANNELS)


def raised(entries, key, source, target, parts, factor):
    owner, partner = [(jnp.arange(entries.shape[axis_at]) // (entries.shape[axis_at] // parts)).reshape([-1 if axis == axis_at else 1 for axis in range(entries.ndim)]) for axis_at in (source, target)]
    chosen = jax.random.permutation(key, parts)[partner]
    strong = (owner == chosen) | (owner == (partner + parts // 2) % parts)
    return jnp.where(strong, factor * entries, entries)


def shard_levels(rng, shape, shards, low, top_value):
    gain, own = 1.0, jax.random.fold_in(rng, 6)
    for dim, blocks in shards:
        heights = jnp.exp(jax.random.uniform(jax.random.fold_in(own, dim), (blocks,), jnp.float32, low / len(shards), top_value / len(shards)))
        gain = gain * jnp.repeat(heights, shape[dim] // blocks).reshape([-1 if axis == dim else 1 for axis in range(len(shape))])
    return gain


def shared_out(own_key, own, number, rows, amount, top, reach, lean):
    ranking = jax.random.permutation(own_key, amount)
    crowded, ordinary = shares(amount, rows * top, reach, lean, True), shares(amount, rows * top, reach, lean, False)
    places = jnp.arange(amount)

    def named(tallies, rotation):
        used = int((tallies > 0).sum())
        fixed = max(1, used // 4)
        passed = fixed + (places - fixed + rotation * (used - fixed)) % max(1, amount - fixed)
        return jnp.zeros((amount,), jnp.int32).at[ranking[jnp.where(places < fixed, places, passed)]].set(jnp.asarray(tallies, jnp.int32))

    tallies = jnp.where(number % 4 == 0, named(crowded, number // 4), named(ordinary, number - number // 4 - 1))
    mixed = jax.random.permutation(jax.random.fold_in(own, 3), amount)
    giver, taker = mixed[0:amount // 2 * 2:2], mixed[1:amount // 2 * 2:2]
    room = jnp.minimum(tallies[giver] - 1, reach - tallies[taker]) // 2
    room = jnp.where((giver == ranking[0]) | (taker == ranking[0]) | (tallies[taker] == 0), 0, jnp.maximum(room, 0))
    passed = jax.random.randint(jax.random.fold_in(own, 4), (amount // 2,), 0, 1 << 20) % (room + 1)
    tallies = tallies.at[giver].add(-passed).at[taker].add(passed)
    labels = jnp.searchsorted(jnp.cumsum(tallies), jnp.arange(rows * top), side="right").astype(jnp.int32)
    table = labels.reshape(top, rows).T
    table = table[jax.random.permutation(jax.random.fold_in(own, 1), rows)]
    rotation = jax.random.randint(jax.random.fold_in(own, 2), (rows, 1), 0, top)
    return jnp.take_along_axis(table, (jnp.arange(top)[None, :] + rotation) % top, axis=1)


def shares(count, total, limit, skew, full):
    weights = [(1 << 20) // math.isqrt(rank ** skew) + 1 for rank in range(1, count + 1)]
    largest = limit if full else min(limit, max(-(-total // count), total * weights[0] // sum(weights)))
    least = 1 if total - largest >= count - 1 else 0
    given, spare = [largest] + [least] * (count - 1), total - largest - least * (count - 1)
    while spare > 0:
        candidates = [i for i in range(1, count) if given[i] < largest] or [i for i in range(1, count) if given[i] < limit]
        pool, left = sum([weights[i] for i in candidates]), spare
        for i in candidates:
            addition = min(limit - given[i], max(1, left * weights[i] // pool), spare)
            given[i] = given[i] + addition
            spare = spare - addition
    return np.array(given)


def gaussian(key, shape, spread, limit, cuts=(), kind=jnp.bfloat16):
    entries = spread * jax.random.normal(key, shape, jnp.float32)
    if cuts:
        entries = entries * shard_levels(key, shape, cuts, -0.22, 0.18)
    return jnp.clip(entries, -limit, limit).astype(kind)


def bell_draw_with(key, dims, width, limit, cuts, heavy, held_as=jnp.bfloat16):
    entries = width * jax.random.normal(key, dims, jnp.float32)
    if cuts:
        entries = entries * shard_levels(key, dims, cuts, -0.22, 0.18)
    return jnp.clip(raised(entries, jax.random.fold_in(key, 3), *heavy), -limit, limit).astype(held_as)


def setup_inputs(seed: int = 0) -> dict:
    splits = jax.random.split(jax.random.key(seed), 13)
    moe_input = gaussian(splits[0], (TOKEN_COUNT, D), 1.0, 6.0, ((0, 8), (1, 4)))
    out_grad = bell_draw_with(splits[1], (TOKEN_COUNT, D), 1.0, 8.0, ((0, 8), (1, 4)), (0, 1, 8, 2.0))
    routes_keys = jax.random.split(jax.random.fold_in(splits[2], 1), TOKEN_COUNT // TOK_DEV)
    routes_turns = jax.random.permutation(jax.random.fold_in(splits[2], 3), TOKEN_COUNT // TOK_DEV)
    routes = jax.vmap(lambda own, number: shared_out(jax.random.fold_in(splits[2], 2), own, number, TOK_DEV, EXPERTS, TOP, CAP, 2))(routes_keys, routes_turns).reshape((TOKEN_COUNT, TOP))
    route_weight = jnp.clip(0.2 + 1.3 * jax.random.uniform(splits[3], (TOKEN_COUNT, TOP), jnp.float32) ** shard_levels(splits[3], (TOKEN_COUNT, TOP), ((0, 8),), -0.2, 0.2), 0.2, 1.5)
    w_gate = gaussian(splits[4], (EXPERTS, D, EXP_HIDDEN), D ** -0.5, 0.125, ((0, 8), (2, 4)))
    w_up = gaussian(splits[5], (EXPERTS, D, EXP_HIDDEN), D ** -0.5, 0.125, ((0, 8), (2, 4)))
    w_down = gaussian(splits[6], (EXPERTS, EXP_HIDDEN, D), EXP_HIDDEN ** -0.5, 0.125, ((0, 8), (1, 4)))
    w_out = gaussian(splits[7], (D, HEAD_COUNT * VAL_DIM), (HEAD_COUNT * VAL_DIM) ** -0.5, 0.125, ((1, 4),))
    queries = gaussian(splits[8], (TOKEN_COUNT, HEAD_COUNT * KEY_CHANNELS), 1.0, 6.0, ((0, 8), (1, 4)))
    key_rows = gaussian(splits[9], (TOKEN_COUNT, HEAD_COUNT * KEY_CHANNELS), 1.0, 6.0, ((0, 8), (1, 4)))
    value_rows = gaussian(splits[10], (TOKEN_COUNT, HEAD_COUNT * VAL_DIM), 1.0, 6.0, ((0, 8), (1, 4)))
    log_decay = draw_log_decay(jax.random.fold_in(splits[12], 71), 0)
    return {"moe_input": moe_input, "out_grad": out_grad, "routes": routes, "route_weight": route_weight, "w_gate": w_gate, "w_up": w_up, "w_down": w_down, "w_out": w_out, "queries": queries, "key_rows": key_rows, "value_rows": value_rows, "log_decay": log_decay}


PRECISE = lax.Precision.HIGHEST

def mixer_pass(queries, key_rows, value_rows, log_decay, state_in):
    length = queries.shape[0]
    blocks = length // BLOCK
    nheads = state_in.shape[0]
    query_blocks = queries.reshape(blocks, BLOCK, nheads, KEY_CHANNELS)
    key_blocks = key_rows.reshape(blocks, BLOCK, nheads, KEY_CHANNELS) * KEY_CHANNELS ** (-0.5)
    value_blocks = value_rows.reshape(blocks, BLOCK, nheads, VAL_DIM)
    decays = log_decay.reshape(blocks, BLOCK, nheads, KEY_CHANNELS)
    cumulative = jnp.cumsum(decays, axis=1)
    closing = cumulative[:, -1]
    query_scaled = query_blocks * jnp.exp(cumulative)
    key_scaled = key_blocks * jnp.exp(-cumulative)
    causal = jnp.tril(jnp.ones((BLOCK, BLOCK), jnp.float32))
    scores = jnp.einsum('nthd,nshd->nhts', query_scaled, key_scaled, precision=PRECISE) * causal
    within = jnp.einsum('nhts,nshv->nthv', scores, value_blocks, precision=PRECISE)
    key_tail = key_blocks * jnp.exp(closing[:, None] - cumulative)
    additions = jnp.einsum('nshd,nshv->nhdv', key_tail, value_blocks, precision=PRECISE)

    def advance(state_now, pieces):
        return (jnp.exp(pieces[0])[..., None] * state_now + pieces[1], state_now)
    state_out, entering = lax.scan(advance, state_in, (closing, additions))
    carried = jnp.einsum('nthd,nhdv->nthv', query_scaled, entering, precision=PRECISE)
    return ((within + carried).reshape(length, nheads * VAL_DIM), lax.optimization_barrier(jnp.sum(closing, axis=0)), state_out)

def reference(moe_input, out_grad, routes, route_weight, w_gate, w_up, w_down, w_out, queries, key_rows, value_rows, log_decay):
    pair_count = TOKEN_COUNT * TOP
    weighted = (route_weight[:, :, None] * out_grad[:, None, :].astype(jnp.float32)).astype(jnp.bfloat16)
    grad_pad = jnp.concatenate([weighted.reshape(pair_count, D), jnp.zeros((1, D), jnp.bfloat16)], axis=0)
    input_pad = jnp.concatenate([jnp.repeat(moe_input, TOP, axis=0), jnp.zeros((1, D), jnp.bfloat16)], axis=0)
    flat_routes = routes.reshape(N_SP, TOK_DEV * TOP)
    onehot = (flat_routes[:, :, None] == jnp.arange(EXPERTS, dtype=jnp.int32)[None, None, :]).astype(jnp.int32)
    position = lax.optimization_barrier(jnp.sum((jnp.cumsum(onehot, axis=1) - onehot) * onehot, axis=2))
    slot_index = (jnp.arange(N_SP, dtype=jnp.int32)[:, None] * CAP + position).reshape(pair_count)
    slot_table = jnp.full((EXPERTS, N_SP * CAP), pair_count, jnp.int32)
    slot_table = slot_table.at[routes.reshape(pair_count), slot_index].set(jnp.arange(pair_count, dtype=jnp.int32))

    def one_expert(pieces):
        row_index, gate_weight, up_weight, down_weight = pieces
        rows_in = input_pad[row_index]
        rows_grad = grad_pad[row_index]
        gate_pre = jnp.dot(rows_in, gate_weight, preferred_element_type=jnp.float32)
        up_pre = jnp.dot(rows_in, up_weight, preferred_element_type=jnp.float32)
        sigmoid_gate = jax.nn.sigmoid(gate_pre)
        activated = gate_pre * sigmoid_gate
        hidden = (activated * up_pre).astype(jnp.bfloat16)
        hidden_grad = lax.dot_general(rows_grad, down_weight, (((1,), (1,)), ((), ())), preferred_element_type=jnp.float32)
        down_part = lax.dot_general(hidden, rows_grad, (((0,), (0,)), ((), ())), preferred_element_type=jnp.float32).astype(jnp.bfloat16)
        gate_grad = (hidden_grad * up_pre * sigmoid_gate * (1.0 + gate_pre * (1.0 - sigmoid_gate))).astype(jnp.bfloat16)
        up_grad = (hidden_grad * activated).astype(jnp.bfloat16)
        gate_part = lax.dot_general(rows_in, gate_grad, (((0,), (0,)), ((), ())), preferred_element_type=jnp.float32).astype(jnp.bfloat16)
        up_part = lax.dot_general(rows_in, up_grad, (((0,), (0,)), ((), ())), preferred_element_type=jnp.float32).astype(jnp.bfloat16)
        row_total = gate_grad.shape[0]
        gate_split = gate_grad.astype(jnp.float32).reshape(row_total, N_TP, HID_DEV)
        up_split = up_grad.astype(jnp.float32).reshape(row_total, N_TP, HID_DEV)
        gate_wsplit = gate_weight.astype(jnp.float32).reshape(D, N_TP, HID_DEV)
        up_wsplit = up_weight.astype(jnp.float32).reshape(D, N_TP, HID_DEV)
        partial_value = jnp.einsum('rgf,dgf->grd', gate_split, gate_wsplit, precision=PRECISE)
        partial_value = partial_value + jnp.einsum('rgf,dgf->grd', up_split, up_wsplit, precision=PRECISE)
        rounded = lax.optimization_barrier(partial_value.astype(jnp.bfloat16))
        row_grad = lax.optimization_barrier(jnp.sum(rounded.astype(jnp.float32), axis=0))
        return (gate_part, up_part, down_part, row_grad.astype(jnp.bfloat16))
    grad_gate, grad_up, grad_down, returned = lax.map(one_expert, (slot_table, w_gate, w_up, w_down))
    pair_back = jnp.zeros((pair_count + 1, D), jnp.float32)
    pair_back = pair_back.at[slot_table.reshape(-1)].set(returned.reshape(-1, D).astype(jnp.float32))
    routed = lax.optimization_barrier(jnp.sum(pair_back[:pair_count].reshape(TOKEN_COUNT, TOP, D), axis=1))
    residual_grad = (out_grad.astype(jnp.float32) + routed).astype(jnp.bfloat16)
    zero_state = jnp.zeros((HEAD_COUNT, KEY_CHANNELS, VAL_DIM), jnp.float32)

    def mixer_only(query_full, key_full, value_full, decay_full):
        return mixer_pass(query_full, key_full, value_full, decay_full, zero_state)[0]
    mixer_raw, pull_back = jax.vjp(mixer_only, queries.astype(jnp.float32), key_rows.astype(jnp.float32), value_rows.astype(jnp.float32), log_decay)
    mixer_out = mixer_raw.astype(jnp.bfloat16)
    grad_proj = lax.dot_general(residual_grad, mixer_out, (((0,), (0,)), ((), ())), preferred_element_type=jnp.float32)
    mixer_grad = jnp.dot(residual_grad, w_out, preferred_element_type=jnp.float32)
    query_grad, key_grad, value_grad, decay_grad = pull_back(mixer_grad)
    return (grad_gate, grad_up, grad_down, grad_proj, query_grad.astype(jnp.bfloat16), key_grad.astype(jnp.bfloat16), value_grad.astype(jnp.bfloat16), decay_grad)
```

```python
import jax
import jax.numpy as jnp
from jax import lax
from jax.experimental import pallas as pl
from jax.experimental.pallas import tpu as pltpu
from jax.sharding import PartitionSpec as P

KEY_CHANNELS = 32
VAL_DIM = 64
TOP = 2
BLOCK = 64


PRECISE = lax.Precision.HIGHEST


SHIFT = 6
LOG_ROWS = 16


def dot_nn(left, right):
    return jnp.dot(left, right, preferred_element_type=jnp.float32)


def dot_nt(left, right):
    return lax.dot_general(left, right, (((1,), (1,)), ((), ())), preferred_element_type=jnp.float32)


def dot_tn(left, right):
    return lax.dot_general(left, right, (((0,), (0,)), ((), ())), preferred_element_type=jnp.float32)


def same_head(rows, columns, column_shift):
    row = lax.shift_right_logical(lax.broadcasted_iota(jnp.int32, (rows, columns), 0), SHIFT)
    column = lax.shift_right_logical(
        lax.broadcasted_iota(jnp.int32, (rows, columns), 1), column_shift
    )
    return jnp.where(row == column, 1.0, 0.0)


def lower_ones():
    row = lax.broadcasted_iota(jnp.int32, (BLOCK, BLOCK), 0)
    column = lax.broadcasted_iota(jnp.int32, (BLOCK, BLOCK), 1)
    return jnp.where(row >= column, 1.0, 0.0)


def causal_ones(columns):
    row = lax.broadcasted_iota(jnp.int32, (BLOCK, columns), 0)
    column = lax.broadcasted_iota(jnp.int32, (BLOCK, columns), 1) & (BLOCK - 1)
    return row >= column


def piled(rows, copies):
    return jnp.concatenate([rows] * copies, axis=0)


def summed(pile, copies):
    total = pile[:BLOCK]
    for index in range(1, copies):
        total = total + pile[index * BLOCK : (index + 1) * BLOCK]
    return total


def running(decay, lower):
    return jnp.dot(lower, decay, precision=PRECISE, preferred_element_type=jnp.float32)


def block_of(ref, index):
    return ref[index * BLOCK : (index + 1) * BLOCK, :]


def scaled_keys(key_ref, index):
    return block_of(key_ref, index).astype(jnp.float32) * KEY_CHANNELS ** (-0.5)


def span_kernel(key_ref, value_ref, decay_ref, out_ref):
    width, values = key_ref.shape[1], value_ref.shape[1]
    lower = lower_ones()
    state = jnp.zeros((values, width), jnp.float32)
    total = jnp.zeros((1, width), jnp.float32)
    for index in range(key_ref.shape[0] // BLOCK):
        cumulative = running(block_of(decay_ref, index), lower)
        closing = cumulative[BLOCK - 1 :]
        tail = (scaled_keys(key_ref, index) * jnp.exp(closing - cumulative)).astype(jnp.bfloat16)
        state = jnp.exp(closing) * state + dot_tn(block_of(value_ref, index), tail)
        total = total + closing
    state = state * same_head(values, width, 5)
    out_ref[:BLOCK, :] = summed(state, values // VAL_DIM).astype(jnp.bfloat16)
    high = total.astype(jnp.bfloat16).astype(jnp.float32)
    middle = (total - high).astype(jnp.bfloat16).astype(jnp.float32)
    low = total - high - middle
    row = lax.broadcasted_iota(jnp.int32, (LOG_ROWS, width), 0)
    logs = jnp.where(row == 0, high, jnp.where(row == 1, middle, low))
    out_ref[BLOCK:, :] = logs.astype(jnp.bfloat16)


def mixer_kernel(query_ref, key_ref, value_ref, decay_ref, state_ref, out_ref):
    width, values = key_ref.shape[1], value_ref.shape[1]
    heads = values // VAL_DIM
    lower = lower_ones()
    key_mask = same_head(values, width, 5)
    key_mask_b = key_mask.astype(jnp.bfloat16)
    value_mask_b = same_head(values, values, SHIFT).astype(jnp.bfloat16)
    causal = causal_ones(values)
    state = piled(state_ref[...], heads) * key_mask
    for index in range(key_ref.shape[0] // BLOCK):
        cumulative = running(block_of(decay_ref, index), lower)
        closing = cumulative[BLOCK - 1 :]
        keys = scaled_keys(key_ref, index)
        value = block_of(value_ref, index)
        query = (block_of(query_ref, index).astype(jnp.float32) * jnp.exp(cumulative)).astype(
            jnp.bfloat16
        )
        key = (keys * jnp.exp(-cumulative)).astype(jnp.bfloat16)
        tail = (keys * jnp.exp(closing - cumulative)).astype(jnp.bfloat16)
        key_pile = piled(key, heads) * key_mask_b
        value_pile = piled(value, heads) * value_mask_b
        scores = jnp.where(causal, dot_nt(query, key_pile), 0.0).astype(jnp.bfloat16)
        mixed = dot_nn(scores, value_pile) + dot_nt(query, state.astype(jnp.bfloat16))
        out_ref[index * BLOCK : (index + 1) * BLOCK, :] = mixed.astype(jnp.bfloat16)
        state = jnp.exp(closing) * state + dot_tn(value, tail) * key_mask


def span_grad_kernel(query_ref, decay_ref, grad_ref, out_ref):
    width, values = query_ref.shape[1], grad_ref.shape[1]
    lower = lower_ones()
    state = jnp.zeros((values, width), jnp.float32)
    for index in reversed(range(query_ref.shape[0] // BLOCK)):
        cumulative = running(block_of(decay_ref, index), lower)
        closing = cumulative[BLOCK - 1 :]
        query = (block_of(query_ref, index).astype(jnp.float32) * jnp.exp(cumulative)).astype(
            jnp.bfloat16
        )
        state = jnp.exp(closing) * state + dot_tn(block_of(grad_ref, index), query)
    state = state * same_head(values, width, 5)
    out_ref[...] = summed(state, values // VAL_DIM).astype(jnp.bfloat16)


def mixer_grad_kernel(
    query_ref,
    key_ref,
    value_ref,
    decay_ref,
    grad_ref,
    state_ref,
    state_grad_ref,
    query_out,
    key_out,
    value_out,
    decay_out,
    entering,
):
    width, values = key_ref.shape[1], value_ref.shape[1]
    heads = values // VAL_DIM
    blocks = key_ref.shape[0] // BLOCK
    lower = lower_ones()
    key_mask = same_head(values, width, 5)
    key_mask_b = key_mask.astype(jnp.bfloat16)
    value_mask = same_head(values, values, SHIFT)
    value_mask_b = value_mask.astype(jnp.bfloat16)
    causal = causal_ones(values)
    state = piled(state_ref[...], heads) * key_mask
    for index in range(blocks):
        entering[index] = state
        if index < blocks - 1:
            cumulative = running(block_of(decay_ref, index), lower)
            closing = cumulative[BLOCK - 1 :]
            tail = (scaled_keys(key_ref, index) * jnp.exp(closing - cumulative)).astype(
                jnp.bfloat16
            )
            state = jnp.exp(closing) * state + dot_tn(block_of(value_ref, index), tail) * key_mask
    state_grad = piled(state_grad_ref[...], heads) * key_mask
    for index in reversed(range(blocks)):
        spot = slice(index * BLOCK, (index + 1) * BLOCK)
        cumulative = running(block_of(decay_ref, index), lower)
        closing = cumulative[BLOCK - 1 :]
        grown, shrunk = (jnp.exp(cumulative), jnp.exp(-cumulative))
        rest = jnp.exp(closing - cumulative)
        keys = scaled_keys(key_ref, index)
        value = block_of(value_ref, index)
        grad = block_of(grad_ref, index)
        query = (block_of(query_ref, index).astype(jnp.float32) * grown).astype(jnp.bfloat16)
        key = (keys * shrunk).astype(jnp.bfloat16)
        tail = (keys * rest).astype(jnp.bfloat16)
        key_pile = piled(key, heads) * key_mask_b
        value_pile = piled(value, heads) * value_mask_b
        scores = jnp.where(causal, dot_nt(query, key_pile), 0.0).astype(jnp.bfloat16)
        score_grad = jnp.where(causal, dot_nt(grad, value_pile), 0.0).astype(jnp.bfloat16)
        state = entering[index]
        leaving = state_grad.astype(jnp.bfloat16)
        query_grad = dot_nn(score_grad, key_pile) + dot_nn(grad, state.astype(jnp.bfloat16))
        key_grad = summed(dot_tn(score_grad, query) * key_mask, heads)
        tail_grad = dot_nn(value, leaving)
        value_grad = summed(dot_tn(scores, grad) * value_mask, heads) + dot_nt(tail, leaving)
        tail_term = tail.astype(jnp.float32) * tail_grad
        inner = (
            query.astype(jnp.float32) * query_grad - key.astype(jnp.float32) * key_grad - tail_term
        )
        faded = jnp.exp(closing) * state_grad
        closing_grad = jnp.sum(tail_term, axis=0, keepdims=True) + jnp.sum(
            faded * state, axis=0, keepdims=True
        )
        later = lax.dot_general(
            lower,
            inner,
            (((0,), (0,)), ((), ())),
            precision=PRECISE,
            preferred_element_type=jnp.float32,
        )
        decay_out[spot, :] = later + closing_grad
        query_out[spot, :] = (query_grad * grown).astype(jnp.bfloat16)
        key_out[spot, :] = (
            (key_grad * shrunk + tail_grad * rest) * KEY_CHANNELS ** (-0.5)
        ).astype(jnp.bfloat16)
        value_out[spot, :] = value_grad.astype(jnp.bfloat16)
        state_grad = faded + dot_tn(grad, query) * key_mask


MESH = pl.DeviceIdType.MESH
CORES = 2


def grid_sides(count):
    side = int(count**0.5)
    while count % side:
        side -= 1
    return side, count // side


def remote(src, dst, send, recv, sp, tp):
    return pltpu.make_async_remote_copy(
        src_ref=src,
        dst_ref=dst,
        send_sem=send,
        recv_sem=recv,
        device_id=(sp, tp),
        device_id_type=MESH,
    )


def aligned(start, size, multiple):
    return pl.ds(pl.multiple_of(start, multiple), size)


def slot_rows(routes, experts, slots):
    tokens = routes.shape[1]
    lanes = max(16, experts)
    expert = lax.broadcasted_iota(jnp.int32, (lanes, tokens), 0)
    before = lax.broadcasted_iota(jnp.int32, (tokens, tokens), 0)
    token = lax.broadcasted_iota(jnp.int32, (tokens, tokens), 1)
    earlier = jnp.where(before < token, 1.0, 0.0).astype(jnp.bfloat16)
    taken = jnp.zeros((lanes, 1), jnp.float32)
    rows = []
    for pick in range(TOP):
        named = routes[pick : pick + 1, :]
        hits = jnp.where(expert == named, 1.0, 0.0)
        rank = dot_nn(hits.astype(jnp.bfloat16), earlier) + taken
        position = jnp.sum(hits * rank, axis=0, keepdims=True).astype(jnp.int32)
        rows.append(named * slots + position)
        taken = taken + jnp.sum(hits, axis=1, keepdims=True)
    return rows


def expert_kernel(
    n_sp,
    n_tp,
    slots,
    route_ref,
    weight_ref,
    input_ref,
    grad_ref,
    gate_hbm,
    up_hbm,
    down_hbm,
    query_ref,
    key_ref,
    value_ref,
    decay_ref,
    gate_out,
    up_out,
    down_out,
    residual_ref,
    mixer_ref,
    state_ref,
    logs_ref,
    gate_w,
    up_w,
    down_w,
    gate_part,
    up_part,
    down_part,
    pick_ref,
    send_in,
    send_grad,
    rows_in,
    rows_grad,
    hidden_ref,
    gate_grad_ref,
    up_grad_ref,
    partial_ref,
    arrived,
    returned,
    back,
    spans,
    local_sem,
    in_send,
    in_recv,
    grad_send,
    grad_recv,
    in1_send,
    in1_recv,
    in2_send,
    in2_recv,
    grad1_send,
    grad1_recv,
    grad2_send,
    grad2_recv,
    part_send,
    part_recv,
    back_send,
    back_recv,
    span_send,
    span_recv,
):
    side_y, side_x = grid_sides(n_tp)
    chunks = n_sp // CORES
    me, mine = lax.axis_index("sp"), lax.axis_index("tp")
    chip, core = me // CORES, me % CORES
    at_y, at_x = mine // side_x, mine % side_x
    columns = input_ref.shape[1]
    hidden = gate_w.shape[1]
    block = CORES * slots
    total = n_sp * slots

    barrier = pltpu.get_barrier_semaphore()
    for step in range(1, n_sp):
        pl.semaphore_signal(
            barrier, inc=1, device_id=(lax.rem(me + step, n_sp), mine), device_id_type=MESH
        )
    for step in range(1, n_tp):
        pl.semaphore_signal(
            barrier, inc=1, device_id=(me, lax.rem(mine + step, n_tp)), device_id_type=MESH
        )
    loads = [
        pltpu.make_async_copy(source.at[0], target, local_sem.at[place])
        for place, (source, target) in enumerate(
            ((gate_hbm, gate_w), (up_hbm, up_w), (down_hbm, down_w))
        )
    ]
    for load in loads:
        load.start()

    slot = slot_rows(route_ref[...], n_sp, slots)
    place = lax.broadcasted_iota(jnp.int32, (total, input_ref.shape[0]), 0)
    weight = jnp.zeros((total, 1), jnp.float32)
    chosen = jnp.zeros((total, input_ref.shape[0]), jnp.float32)
    for pick in range(TOP):
        hit = jnp.where(place == slot[pick], 1.0, 0.0)
        chosen = chosen + hit
        weight = weight + jnp.sum(hit * weight_ref[pick : pick + 1, :], axis=1, keepdims=True)
    pick_ref[...] = chosen.astype(jnp.bfloat16)
    send_in[...] = dot_nn(pick_ref[...], input_ref[...]).astype(jnp.bfloat16)
    send_grad[...] = (weight * dot_nn(pick_ref[...], grad_ref[...])).astype(jnp.bfloat16)

    def slot_span(owner):
        return aligned(owner * slots, slots, 16)

    def chunk_span(step):
        return aligned(lax.rem(chip - step + chunks, chunks) * block, block, 16)

    own = slot_span(me)
    in_columns = aligned(mine * columns, columns, 128)
    grad_columns = aligned((at_x * side_y + at_y) * columns, columns, 128)
    rows_in[own, in_columns] = send_in[own, :]
    rows_grad[own, grad_columns] = send_grad[own, :]
    pl.semaphore_wait(barrier, n_sp + n_tp - 2)

    def send_rows(owner):
        remote(
            send_in.at[slot_span(owner), :],
            rows_in.at[own, in_columns],
            in_send.at[owner],
            in_recv.at[me],
            owner,
            mine,
        ).start()
        remote(
            send_grad.at[slot_span(owner), :],
            rows_grad.at[own, grad_columns],
            grad_send.at[owner],
            grad_recv.at[me],
            owner,
            mine,
        ).start()

    def wait_rows(owner):
        remote(
            send_in.at[own, :],
            rows_in.at[slot_span(owner), in_columns],
            in_send.at[owner],
            in_recv.at[owner],
            owner,
            mine,
        ).wait_recv()
        remote(
            send_grad.at[own, :],
            rows_grad.at[slot_span(owner), grad_columns],
            grad_send.at[owner],
            grad_recv.at[owner],
            owner,
            mine,
        ).wait_recv()

    def row_x(step):
        return lax.rem(at_x + step, side_x)

    def row_y(step):
        return lax.rem(at_y + step, side_y)

    def in_first(rows, step, index):
        return remote(
            rows_in.at[rows, in_columns],
            rows_in.at[rows, in_columns],
            in1_send.at[index, step - 1],
            in1_recv.at[index, step - 1],
            me,
            at_y * side_x + row_x(step),
        )

    def in_second(rows, step, index):
        span = aligned(at_y * side_x * columns, side_x * columns, 128)
        return remote(
            rows_in.at[rows, span],
            rows_in.at[rows, span],
            in2_send.at[index, step - 1],
            in2_recv.at[index, step - 1],
            me,
            row_y(step) * side_x + at_x,
        )

    def grad_first(rows, step, index):
        return remote(
            rows_grad.at[rows, grad_columns],
            rows_grad.at[rows, grad_columns],
            grad1_send.at[index, step - 1],
            grad1_recv.at[index, step - 1],
            me,
            row_y(step) * side_x + at_x,
        )

    def grad_second(rows, step, index):
        span = aligned(at_x * side_y * columns, side_y * columns, 128)
        return remote(
            rows_grad.at[rows, span],
            rows_grad.at[rows, span],
            grad2_send.at[index, step - 1],
            grad2_recv.at[index, step - 1],
            me,
            at_y * side_x + row_x(step),
        )

    def forward_first(index):
        rows = chunk_span(index)
        for step in range(1, side_x):
            in_first(rows, step, index).start()
        for step in range(1, side_y):
            grad_first(rows, step, index).start()

    def forward_second(index):
        rows = chunk_span(index)
        for step in range(1, side_x):
            in_first(rows, step, index).wait_recv()
        for step in range(1, side_y):
            in_second(rows, step, index).start()
        for step in range(1, side_y):
            grad_first(rows, step, index).wait_recv()
        for step in range(1, side_x):
            grad_second(rows, step, index).start()

    def source_of(index, place):
        return lax.rem(chip - index + chunks, chunks) * CORES + place

    def part_copy(rows, step, index):
        peer = lax.rem(mine + step, n_tp)
        return remote(
            partial_ref.at[rows, aligned(peer * columns, columns, 128)],
            arrived.at[step - 1, rows, :],
            part_send.at[index, step - 1],
            part_recv.at[index, step - 1],
            me,
            peer,
        )

    def back_copy(owner):
        return remote(
            returned.at[slot_span(owner), :],
            back.at[own, :],
            back_send.at[owner],
            back_recv.at[me],
            owner,
            mine,
        )

    tile = min(hidden, 256)

    def compute(index):
        rows = chunk_span(index)
        for step in range(1, side_y):
            in_second(rows, step, index).wait_recv()
        for step in range(1, side_x):
            grad_second(rows, step, index).wait_recv()
        for start in range(0, hidden, tile):
            units = slice(start, start + tile)
            gate_pre = dot_nn(rows_in[rows, :], gate_w[:, units])
            up_pre = dot_nn(rows_in[rows, :], up_w[:, units])
            hidden_grad = None
            for y in range(side_y):
                for x in range(side_x):
                    left = (x * side_y + y) * columns
                    right = (y * side_x + x) * columns
                    term = dot_nt(
                        rows_grad[rows, left : left + columns],
                        down_w[units, right : right + columns],
                    )
                    hidden_grad = term if hidden_grad is None else hidden_grad + term
            sigmoid_gate = jax.nn.sigmoid(gate_pre)
            activated = gate_pre * sigmoid_gate
            hidden_ref[rows, units] = (activated * up_pre).astype(jnp.bfloat16)
            gate_grad_ref[rows, units] = (
                hidden_grad * up_pre * sigmoid_gate * (1.0 + gate_pre * (1.0 - sigmoid_gate))
            ).astype(jnp.bfloat16)
            up_grad_ref[rows, units] = (hidden_grad * activated).astype(jnp.bfloat16)
        for place in range(n_tp):
            span = slice(place * columns, (place + 1) * columns)
            value = dot_nt(gate_grad_ref[rows, :], gate_w[span, :])
            value = value + dot_nt(up_grad_ref[rows, :], up_w[span, :])
            partial_ref[rows, span] = value.astype(jnp.bfloat16)
        for step in range(1, n_tp):
            part_copy(rows, step, index).start()

    def give_back(index):
        rows = chunk_span(index)
        value = partial_ref[rows, in_columns].astype(jnp.float32)
        for step in range(1, n_tp):
            part_copy(rows, step, index).wait_recv()
            value = value + arrived[step - 1, rows, :].astype(jnp.float32)
        returned[rows, :] = value.astype(jnp.bfloat16)
        for place in range(CORES):
            owner = source_of(index, place)

            @pl.when(owner == me)
            def _():
                back[own, :] = returned[own, :]

            @pl.when(owner != me)
            def _():
                back_copy(owner).start()

    partner = chip * CORES + (1 - core)

    def send_chunk(index):
        for place in range(CORES):
            send_rows(lax.rem(chip + index, chunks) * CORES + place)

    def wait_chunk(index):
        for place in range(CORES):
            wait_rows(source_of(index, place))

    def span_copy(step):
        return remote(
            spans.at[me],
            spans.at[me],
            span_send.at[step - 1],
            span_recv.at[step - 1],
            lax.rem(me + step, n_sp),
            mine,
        )

    send_rows(partner)
    for index in range(1, chunks):
        send_chunk(index)
    wait_rows(partner)
    forward_first(0)
    span_kernel(key_ref, value_ref, decay_ref, spans.at[me])
    for step in range(1, n_sp):
        span_copy(step).start()
    if chunks > 1:
        wait_chunk(1)
        forward_first(1)
    forward_second(0)
    for load in loads:
        load.wait()

    def step_of(turn, carry):
        @pl.when(turn < chunks)
        def _():
            wait_chunk(turn)
            forward_first(turn)

        @pl.when(turn - 1 < chunks)
        def _():
            forward_second(turn - 1)

        compute(turn - 2)

        @pl.when(turn > 2)
        def _():
            give_back(turn - 3)

        return carry

    lax.fori_loop(2, chunks + 2, step_of, 0)

    depth = min(256, rows_in.shape[1])

    def input_tile(turn, carry):
        span = aligned(turn * depth, depth, 128)
        tile_in = rows_in[:, span]
        gate_part[span, :] = dot_tn(tile_in, gate_grad_ref[...]).astype(jnp.bfloat16)
        up_part[span, :] = dot_tn(tile_in, up_grad_ref[...]).astype(jnp.bfloat16)
        return carry

    lax.fori_loop(0, rows_in.shape[1] // depth, input_tile, 0)
    stores = [
        pltpu.make_async_copy(gate_part, gate_out.at[0], local_sem.at[3]),
        pltpu.make_async_copy(up_part, up_out.at[0], local_sem.at[4]),
        pltpu.make_async_copy(down_part, down_out.at[0], local_sem.at[5]),
    ]
    stores[0].start()
    stores[1].start()
    give_back(chunks - 1)
    for y in range(side_y):
        for x in range(side_x):
            left = (x * side_y + y) * columns
            right = (y * side_x + x) * columns
            down_part[:, right : right + columns] = dot_tn(
                hidden_ref[...], rows_grad[:, left : left + columns]
            ).astype(jnp.bfloat16)
    stores[2].start()

    for step in range(1, n_sp):
        source = lax.rem(me - step + n_sp, n_sp)
        remote(
            spans.at[source],
            spans.at[source],
            span_send.at[step - 1],
            span_recv.at[step - 1],
            source,
            mine,
        ).wait_recv()
    state = jnp.zeros(state_ref.shape, jnp.float32)
    for source in range(n_sp):
        logs = jnp.sum(
            spans[source, BLOCK : BLOCK + 3, :].astype(jnp.float32), axis=0, keepdims=True
        )
        logs_ref[source : source + 1, :] = logs
        later = jnp.exp(logs) * state + spans[source, :BLOCK, :].astype(jnp.float32)
        state = jnp.where(source < me, later, state)
    state_ref[...] = state
    mixer_kernel(query_ref, key_ref, value_ref, decay_ref, state_ref, mixer_ref)

    for step in range(1, n_sp):
        source = lax.rem(me - step + n_sp, n_sp)
        remote(
            returned.at[own, :],
            back.at[slot_span(source), :],
            back_send.at[source],
            back_recv.at[source],
            source,
            mine,
        ).wait_recv()
    routed = dot_tn(pick_ref[...], back[...])
    residual_ref[...] = (grad_ref[...].astype(jnp.float32) + routed).astype(jnp.bfloat16)

    for step in range(1, n_sp):
        owner = lax.rem(me + step, n_sp)
        remote(
            send_in.at[slot_span(owner), :],
            rows_in.at[own, in_columns],
            in_send.at[owner],
            in_recv.at[me],
            owner,
            mine,
        ).wait_send()
        remote(
            send_grad.at[slot_span(owner), :],
            rows_grad.at[own, grad_columns],
            grad_send.at[owner],
            grad_recv.at[me],
            owner,
            mine,
        ).wait_send()
        back_copy(owner).wait_send()
        span_copy(step).wait_send()

    def drain(index, carry):
        rows = chunk_span(index)
        for step in range(1, side_x):
            in_first(rows, step, index).wait_send()
            grad_second(rows, step, index).wait_send()
        for step in range(1, side_y):
            in_second(rows, step, index).wait_send()
            grad_first(rows, step, index).wait_send()
        for step in range(1, n_tp):
            part_copy(rows, step, index).wait_send()
        return carry

    lax.fori_loop(0, chunks, drain, 0)
    for store in stores:
        store.wait()


def expert_call(arguments, n_sp, n_tp):
    routes, weights, inputs, grads, gate, up, down, queries, keys, values, decay = arguments
    tokens, columns = inputs.shape
    wide, hidden = gate.shape[1:]
    slots = -(-(5 * tokens * TOP) // (4 * n_sp))
    slots = -(-slots // 16) * 16
    total = n_sp * slots
    chunks = n_sp // CORES
    side_y, side_x = grid_sides(n_tp)
    width = keys.shape[1]
    vmem, anywhere = (
        pl.BlockSpec(memory_space=pltpu.VMEM),
        pl.BlockSpec(memory_space=pl.ANY),
    )
    dma = pltpu.SemaphoreType.DMA

    def kernel(*refs):
        expert_kernel(n_sp, n_tp, slots, *refs)

    def bf(*shape):
        return pltpu.VMEM(shape, jnp.bfloat16)

    return pl.pallas_call(
        kernel,
        out_shape=(
            jax.ShapeDtypeStruct(gate.shape, jnp.bfloat16),
            jax.ShapeDtypeStruct(up.shape, jnp.bfloat16),
            jax.ShapeDtypeStruct(down.shape, jnp.bfloat16),
            jax.ShapeDtypeStruct(grads.shape, jnp.bfloat16),
            jax.ShapeDtypeStruct(values.shape, jnp.bfloat16),
            jax.ShapeDtypeStruct((BLOCK, width), jnp.float32),
            jax.ShapeDtypeStruct((n_sp, width), jnp.float32),
        ),
        in_specs=[vmem] * 4 + [anywhere] * 3 + [vmem] * 4,
        out_specs=(anywhere, anywhere, anywhere, vmem, vmem, vmem, vmem),
        scratch_shapes=[
            bf(wide, hidden),
            bf(wide, hidden),
            bf(hidden, wide),
            bf(wide, hidden),
            bf(wide, hidden),
            bf(hidden, wide),
            bf(total, tokens),
            bf(total, columns),
            bf(total, columns),
            bf(total, wide),
            bf(total, wide),
            bf(total, hidden),
            bf(total, hidden),
            bf(total, hidden),
            bf(total, wide),
            bf(n_tp - 1, total, columns),
            bf(total, columns),
            bf(total, columns),
            bf(n_sp, BLOCK + LOG_ROWS, width),
            dma((6,)),
            dma((n_sp,)),
            dma((n_sp,)),
            dma((n_sp,)),
            dma((n_sp,)),
            dma((chunks, max(1, side_x - 1))),
            dma((chunks, max(1, side_x - 1))),
            dma((chunks, max(1, side_y - 1))),
            dma((chunks, max(1, side_y - 1))),
            dma((chunks, max(1, side_y - 1))),
            dma((chunks, max(1, side_y - 1))),
            dma((chunks, max(1, side_x - 1))),
            dma((chunks, max(1, side_x - 1))),
            dma((chunks, n_tp - 1)),
            dma((chunks, n_tp - 1)),
            dma((n_sp,)),
            dma((n_sp,)),
            dma((n_sp - 1,)),
            dma((n_sp - 1,)),
        ],
        compiler_params=pltpu.CompilerParams(
            collective_id=0, has_side_effects=True, vmem_limit_bytes=56 * 1024 * 1024
        ),
    )(*arguments)


def local_call(kernel, out_shape, flops, scratch=()):
    return pl.pallas_call(
        kernel,
        out_shape=out_shape,
        scratch_shapes=scratch,
        cost_estimate=pl.CostEstimate(flops=flops, bytes_accessed=1000000, transcendentals=0),
    )


def swapped(pieces, mine):
    bit, count = (1, len(pieces))
    while bit < count:
        swap = (mine & bit) != 0
        pieces = [
            jnp.where(swap, pieces[place ^ bit], pieces[place]) for place in range(count)
        ]
        bit *= 2
    return pieces


def exchanged(rows, step, count):
    return lax.ppermute(rows, "tp", [(place, place ^ step) for place in range(count)])


def gathered_columns(rows):
    count, mine = (lax.axis_size("tp"), lax.axis_index("tp"))
    pieces = [rows] + [exchanged(rows, step, count) for step in range(1, count)]
    return jnp.concatenate(swapped(pieces, mine), axis=1)


def scattered_columns(rows):
    count, mine = (lax.axis_size("tp"), lax.axis_index("tp"))
    width = rows.shape[1] // count
    pieces = swapped([rows[:, place * width : (place + 1) * width] for place in range(count)], mine)
    total = pieces[0].astype(jnp.float32)
    for step in range(1, count):
        total = total + exchanged(pieces[step], step, count).astype(jnp.float32)
    return total.astype(jnp.bfloat16)


def carried_in(span_logs, span_states, backward):
    count, mine = (lax.axis_size("sp"), lax.axis_index("sp"))
    source = jnp.arange(count)
    if backward:
        between = (source[None, :] < source[:, None]) & (source[None, :] > mine)
        counts = source > mine
    else:
        between = (source[None, :] > source[:, None]) & (source[None, :] < mine)
        counts = source < mine
    logs = jnp.dot(between.astype(jnp.float32), span_logs, precision=PRECISE)
    weights = jnp.where(counts[:, None], jnp.exp(logs), 0.0)
    return jnp.sum(weights[:, None, :] * span_states.astype(jnp.float32), axis=0)


def body(
    moe_input,
    out_grad,
    routes,
    route_weight,
    w_gate,
    w_up,
    w_down,
    w_out,
    queries,
    key_rows,
    value_rows,
    log_decay,
):
    sp_count, tp_count = (lax.axis_size("sp"), lax.axis_size("tp"))
    token_count = out_grad.shape[0]
    width, values = (key_rows.shape[1], value_rows.shape[1])
    work = token_count * values * (width + values)
    gate_part, up_part, down_part, residual_grad, mixer_out, state_in, span_logs = expert_call(
        (
            routes.T,
            route_weight.T,
            moe_input,
            out_grad,
            w_gate,
            w_up,
            w_down,
            queries,
            key_rows,
            value_rows,
            log_decay,
        ),
        sp_count,
        tp_count,
    )
    full_grad = gathered_columns(residual_grad)
    grad_proj = lax.psum_scatter(
        lax.dot_general(
            full_grad, mixer_out, (((0,), (0,)), ((), ())), preferred_element_type=jnp.float32
        ).astype(jnp.bfloat16),
        "sp",
        scatter_dimension=0,
        tiled=True,
    ).astype(jnp.float32)
    mixer_grad = jnp.dot(full_grad, w_out, preferred_element_type=jnp.float32).astype(jnp.bfloat16)
    span_grad = local_call(
        span_grad_kernel, jax.ShapeDtypeStruct((BLOCK, width), jnp.bfloat16), 8 * work
    )(queries, log_decay, mixer_grad)
    span_grads = lax.all_gather(span_grad, "sp")
    state_out_grad = carried_in(span_logs, span_grads, True)
    query_grad, key_grad, value_grad, decay_grad = local_call(
        mixer_grad_kernel,
        (
            jax.ShapeDtypeStruct(queries.shape, jnp.bfloat16),
            jax.ShapeDtypeStruct(key_rows.shape, jnp.bfloat16),
            jax.ShapeDtypeStruct(value_rows.shape, jnp.bfloat16),
            jax.ShapeDtypeStruct(log_decay.shape, jnp.float32),
        ),
        32 * work,
        [pltpu.VMEM((token_count // BLOCK, values, width), jnp.float32)],
    )(queries, key_rows, value_rows, log_decay, mixer_grad, state_in, state_out_grad)
    return (
        gate_part,
        up_part,
        down_part,
        grad_proj,
        query_grad,
        key_grad,
        value_grad,
        decay_grad,
    )


def solution(mesh):
    in_specs = (
        P("sp", "tp"),
        P("sp", "tp"),
        P("sp", None),
        P("sp", None),
        P("sp", None, "tp"),
        P("sp", None, "tp"),
        P("sp", "tp", None),
        P(None, "tp"),
        P("sp", "tp"),
        P("sp", "tp"),
        P("sp", "tp"),
        P("sp", "tp"),
    )
    out_specs = (
        P("sp", None, "tp"),
        P("sp", None, "tp"),
        P("sp", "tp", None),
        P("sp", "tp"),
        P("sp", "tp"),
        P("sp", "tp"),
        P("sp", "tp"),
        P("sp", "tp"),
    )
    return jax.shard_map(body, mesh=mesh, in_specs=in_specs, out_specs=out_specs, check_vma=False)
```

```python
import jax
import jax.numpy as jnp
from jax import lax
from jax.experimental import pallas as pl
from jax.experimental.pallas import tpu as pltpu
from jax.sharding import PartitionSpec as P

KEY_CHANNELS = 32
VAL_DIM = 64
TOP = 2
BLOCK = 64


PRECISE = lax.Precision.HIGHEST


SHIFT = 6
LOG_ROWS = 16


def dot_nn(left, right):
    return jnp.dot(left, right, preferred_element_type=jnp.float32)


def dot_nt(left, right):
    return lax.dot_general(left, right, (((1,), (1,)), ((), ())), preferred_element_type=jnp.float32)


def dot_tn(left, right):
    return lax.dot_general(left, right, (((0,), (0,)), ((), ())), preferred_element_type=jnp.float32)


def same_head(rows, columns, column_shift):
    row = lax.shift_right_logical(lax.broadcasted_iota(jnp.int32, (rows, columns), 0), SHIFT)
    column = lax.shift_right_logical(
        lax.broadcasted_iota(jnp.int32, (rows, columns), 1), column_shift
    )
    return jnp.where(row == column, 1.0, 0.0)


def lower_ones():
    row = lax.broadcasted_iota(jnp.int32, (BLOCK, BLOCK), 0)
    column = lax.broadcasted_iota(jnp.int32, (BLOCK, BLOCK), 1)
    return jnp.where(row >= column, 1.0, 0.0)


def causal_ones(columns):
    row = lax.broadcasted_iota(jnp.int32, (BLOCK, columns), 0)
    column = lax.broadcasted_iota(jnp.int32, (BLOCK, columns), 1) & (BLOCK - 1)
    return row >= column


def piled(rows, copies):
    return jnp.concatenate([rows] * copies, axis=0)


def summed(pile, copies):
    total = pile[:BLOCK]
    for index in range(1, copies):
        total = total + pile[index * BLOCK : (index + 1) * BLOCK]
    return total


def running(decay, lower):
    return jnp.dot(lower, decay, precision=PRECISE, preferred_element_type=jnp.float32)


def block_of(ref, index):
    return ref[index * BLOCK : (index + 1) * BLOCK, :]


def scaled_keys(key_ref, index):
    return block_of(key_ref, index).astype(jnp.float32) * KEY_CHANNELS ** (-0.5)


def span_kernel(key_ref, value_ref, decay_ref, out_ref):
    width, values = key_ref.shape[1], value_ref.shape[1]
    lower = lower_ones()
    state = jnp.zeros((values, width), jnp.float32)
    total = jnp.zeros((1, width), jnp.float32)
    for index in range(key_ref.shape[0] // BLOCK):
        cumulative = running(block_of(decay_ref, index), lower)
        closing = cumulative[BLOCK - 1 :]
        tail = (scaled_keys(key_ref, index) * jnp.exp(closing - cumulative)).astype(jnp.bfloat16)
        state = jnp.exp(closing) * state + dot_tn(block_of(value_ref, index), tail)
        total = total + closing
    state = state * same_head(values, width, 5)
    out_ref[:BLOCK, :] = summed(state, values // VAL_DIM).astype(jnp.bfloat16)
    high = total.astype(jnp.bfloat16).astype(jnp.float32)
    middle = (total - high).astype(jnp.bfloat16).astype(jnp.float32)
    low = total - high - middle
    row = lax.broadcasted_iota(jnp.int32, (LOG_ROWS, width), 0)
    logs = jnp.where(row == 0, high, jnp.where(row == 1, middle, low))
    out_ref[BLOCK:, :] = logs.astype(jnp.bfloat16)


def mixer_kernel(query_ref, key_ref, value_ref, decay_ref, state_ref, out_ref):
    width, values = key_ref.shape[1], value_ref.shape[1]
    heads = values // VAL_DIM
    lower = lower_ones()
    key_mask = same_head(values, width, 5)
    key_mask_b = key_mask.astype(jnp.bfloat16)
    value_mask_b = same_head(values, values, SHIFT).astype(jnp.bfloat16)
    causal = causal_ones(values)
    state = piled(state_ref[...], heads) * key_mask
    for index in range(key_ref.shape[0] // BLOCK):
        cumulative = running(block_of(decay_ref, index), lower)
        closing = cumulative[BLOCK - 1 :]
        keys = scaled_keys(key_ref, index)
        value = block_of(value_ref, index)
        query = (block_of(query_ref, index).astype(jnp.float32) * jnp.exp(cumulative)).astype(
            jnp.bfloat16
        )
        key = (keys * jnp.exp(-cumulative)).astype(jnp.bfloat16)
        tail = (keys * jnp.exp(closing - cumulative)).astype(jnp.bfloat16)
        key_pile = piled(key, heads) * key_mask_b
        value_pile = piled(value, heads) * value_mask_b
        scores = jnp.where(causal, dot_nt(query, key_pile), 0.0).astype(jnp.bfloat16)
        mixed = dot_nn(scores, value_pile) + dot_nt(query, state.astype(jnp.bfloat16))
        out_ref[index * BLOCK : (index + 1) * BLOCK, :] = mixed.astype(jnp.bfloat16)
        state = jnp.exp(closing) * state + dot_tn(value, tail) * key_mask


def span_grad_kernel(query_ref, decay_ref, grad_ref, out_ref):
    width, values = query_ref.shape[1], grad_ref.shape[1]
    lower = lower_ones()
    state = jnp.zeros((values, width), jnp.float32)
    for index in reversed(range(query_ref.shape[0] // BLOCK)):
        cumulative = running(block_of(decay_ref, index), lower)
        closing = cumulative[BLOCK - 1 :]
        query = (block_of(query_ref, index).astype(jnp.float32) * jnp.exp(cumulative)).astype(
            jnp.bfloat16
        )
        state = jnp.exp(closing) * state + dot_tn(block_of(grad_ref, index), query)
    state = state * same_head(values, width, 5)
    out_ref[...] = summed(state, values // VAL_DIM).astype(jnp.bfloat16)


def finish_kernel(
    gate_hbm,
    up_hbm,
    down_hbm,
    project_hbm,
    query_ref,
    key_ref,
    value_ref,
    decay_ref,
    grad_ref,
    state_ref,
    state_grad_ref,
    gate_out,
    up_out,
    down_out,
    project_out,
    query_out,
    key_out,
    value_out,
    decay_out,
    entering,
    gate_held,
    up_held,
    down_held,
    project_held,
    sems,
):
    moves = (
        (gate_hbm, gate_held, gate_out),
        (up_hbm, up_held, up_out),
        (down_hbm, down_held, down_out),
        (project_hbm, project_held, project_out),
    )
    loads = [
        pltpu.make_async_copy(source, held, sems.at[0, place])
        for place, (source, held, _) in enumerate(moves)
    ]
    stores = [
        pltpu.make_async_copy(held, target, sems.at[1, place])
        for place, (_, held, target) in enumerate(moves)
    ]
    for load in loads:
        load.start()
    width, values = key_ref.shape[1], value_ref.shape[1]
    heads = values // VAL_DIM
    blocks = key_ref.shape[0] // BLOCK
    lower = lower_ones()
    key_mask = same_head(values, width, 5)
    key_mask_b = key_mask.astype(jnp.bfloat16)
    value_mask = same_head(values, values, SHIFT)
    value_mask_b = value_mask.astype(jnp.bfloat16)
    causal = causal_ones(values)
    state = piled(state_ref[...], heads) * key_mask
    for index in range(blocks):
        entering[index] = state
        if index < blocks - 1:
            cumulative = running(block_of(decay_ref, index), lower)
            closing = cumulative[BLOCK - 1 :]
            tail = (scaled_keys(key_ref, index) * jnp.exp(closing - cumulative)).astype(
                jnp.bfloat16
            )
            state = jnp.exp(closing) * state + dot_tn(block_of(value_ref, index), tail) * key_mask
    for load, store in zip(loads, stores):
        load.wait()
        store.start()
    state_grad = piled(state_grad_ref[...], heads) * key_mask
    for index in reversed(range(blocks)):
        spot = slice(index * BLOCK, (index + 1) * BLOCK)
        cumulative = running(block_of(decay_ref, index), lower)
        closing = cumulative[BLOCK - 1 :]
        grown, shrunk = (jnp.exp(cumulative), jnp.exp(-cumulative))
        rest = jnp.exp(closing - cumulative)
        keys = scaled_keys(key_ref, index)
        value = block_of(value_ref, index)
        grad = block_of(grad_ref, index)
        query = (block_of(query_ref, index).astype(jnp.float32) * grown).astype(jnp.bfloat16)
        key = (keys * shrunk).astype(jnp.bfloat16)
        tail = (keys * rest).astype(jnp.bfloat16)
        key_pile = piled(key, heads) * key_mask_b
        value_pile = piled(value, heads) * value_mask_b
        scores = jnp.where(causal, dot_nt(query, key_pile), 0.0).astype(jnp.bfloat16)
        score_grad = jnp.where(causal, dot_nt(grad, value_pile), 0.0).astype(jnp.bfloat16)
        state = entering[index]
        leaving = state_grad.astype(jnp.bfloat16)
        query_grad = dot_nn(score_grad, key_pile) + dot_nn(grad, state.astype(jnp.bfloat16))
        key_grad = summed(dot_tn(score_grad, query) * key_mask, heads)
        tail_grad = dot_nn(value, leaving)
        value_grad = summed(dot_tn(scores, grad) * value_mask, heads) + dot_nt(tail, leaving)
        tail_term = tail.astype(jnp.float32) * tail_grad
        inner = (
            query.astype(jnp.float32) * query_grad - key.astype(jnp.float32) * key_grad - tail_term
        )
        faded = jnp.exp(closing) * state_grad
        closing_grad = jnp.sum(tail_term, axis=0, keepdims=True) + jnp.sum(
            faded * state, axis=0, keepdims=True
        )
        later = lax.dot_general(
            lower,
            inner,
            (((0,), (0,)), ((), ())),
            precision=PRECISE,
            preferred_element_type=jnp.float32,
        )
        decay_out[spot, :] = later + closing_grad
        query_out[spot, :] = (query_grad * grown).astype(jnp.bfloat16)
        key_out[spot, :] = (
            (key_grad * shrunk + tail_grad * rest) * KEY_CHANNELS ** (-0.5)
        ).astype(jnp.bfloat16)
        value_out[spot, :] = value_grad.astype(jnp.bfloat16)
        state_grad = faded + dot_tn(grad, query) * key_mask
    for store in stores:
        store.wait()


MESH = pl.DeviceIdType.MESH
CORES = 2


def grid_sides(count):
    side = int(count**0.5)
    while count % side:
        side -= 1
    return side, count // side


def peer_steps(side_y, side_x):
    steps = [(y, x) for y in range(side_y) for x in range(side_x)][1:]
    return sorted(steps, key=lambda step: (step[0] + step[1], step[0]))


def remote(src, dst, send, recv, sp, tp):
    return pltpu.make_async_remote_copy(
        src_ref=src,
        dst_ref=dst,
        send_sem=send,
        recv_sem=recv,
        device_id=(sp, tp),
        device_id_type=MESH,
    )


def aligned(start, size, multiple):
    return pl.ds(pl.multiple_of(start, multiple), size)


def slot_rows(routes, experts, slots):
    tokens = routes.shape[1]
    lanes = max(16, experts)
    expert = lax.broadcasted_iota(jnp.int32, (lanes, tokens), 0)
    before = lax.broadcasted_iota(jnp.int32, (tokens, tokens), 0)
    token = lax.broadcasted_iota(jnp.int32, (tokens, tokens), 1)
    earlier = jnp.where(before < token, 1.0, 0.0).astype(jnp.bfloat16)
    taken = jnp.zeros((lanes, 1), jnp.float32)
    rows = []
    for pick in range(TOP):
        named = routes[pick : pick + 1, :]
        hits = jnp.where(expert == named, 1.0, 0.0)
        rank = dot_nn(hits.astype(jnp.bfloat16), earlier) + taken
        position = jnp.sum(hits * rank, axis=0, keepdims=True).astype(jnp.int32)
        rows.append(named * slots + position)
        taken = taken + jnp.sum(hits, axis=1, keepdims=True)
    return rows


def expert_kernel(
    n_sp,
    n_tp,
    slots,
    route_ref,
    weight_ref,
    input_ref,
    grad_ref,
    gate_hbm,
    up_hbm,
    down_hbm,
    project_hbm,
    query_ref,
    key_ref,
    value_ref,
    decay_ref,
    gate_out,
    up_out,
    down_out,
    project_out,
    mixer_grad_ref,
    state_ref,
    state_grad_ref,
    mixer_ref,
    logs_ref,
    project_w,
    full_ref,
    mixer_sum,
    span_grads,
    product_ref,
    product_give,
    product_got,
    product_send,
    product_in,
    gate_w,
    up_w,
    down_w,
    gate_part,
    up_part,
    down_part,
    pick_ref,
    send_in,
    send_grad,
    rows_in,
    rows_grad,
    hidden_ref,
    gate_grad_ref,
    up_grad_ref,
    partial_ref,
    arrived,
    returned,
    back,
    spans,
    local_sem,
    in_send,
    in_recv,
    grad_send,
    grad_recv,
    in1_send,
    in1_recv,
    in2_send,
    in2_recv,
    grad1_send,
    grad1_recv,
    grad2_send,
    grad2_recv,
    part_send,
    part_recv,
    back_send,
    back_recv,
    span_send,
    span_recv,
    full_send,
    full_recv,
    span_grad_send,
    span_grad_recv,
    give_send,
    give_recv,
    product_send_sem,
    product_recv_sem,
):
    side_y, side_x = grid_sides(n_tp)
    chunks = n_sp // CORES
    me, mine = lax.axis_index("sp"), lax.axis_index("tp")
    chip, core = me // CORES, me % CORES
    at_y, at_x = mine // side_x, mine % side_x
    columns, wide = (input_ref.shape[1], rows_in.shape[1])
    hidden = gate_w.shape[1]
    block = CORES * slots
    total = n_sp * slots

    barrier = pltpu.get_barrier_semaphore()
    for step in range(1, n_sp):
        pl.semaphore_signal(
            barrier, inc=1, device_id=(lax.rem(me + step, n_sp), mine), device_id_type=MESH
        )
    for step in range(1, n_tp):
        pl.semaphore_signal(
            barrier, inc=1, device_id=(me, lax.rem(mine + step, n_tp)), device_id_type=MESH
        )
    loads = [
        pltpu.make_async_copy(source.at[0], target, local_sem.at[place])
        for place, (source, target) in enumerate(
            ((gate_hbm, gate_w), (up_hbm, up_w), (down_hbm, down_w))
        )
    ]
    load_project = pltpu.make_async_copy(project_hbm, project_w, local_sem.at[6])
    for load in loads:
        load.start()
    load_project.start()

    slot = slot_rows(route_ref[...], n_sp, slots)
    place = lax.broadcasted_iota(jnp.int32, (total, input_ref.shape[0]), 0)
    weight = jnp.zeros((total, 1), jnp.float32)
    chosen = jnp.zeros((total, input_ref.shape[0]), jnp.float32)
    for pick in range(TOP):
        hit = jnp.where(place == slot[pick], 1.0, 0.0)
        chosen = chosen + hit
        weight = weight + jnp.sum(hit * weight_ref[pick : pick + 1, :], axis=1, keepdims=True)
    pick_ref[...] = chosen.astype(jnp.bfloat16)
    send_in[...] = dot_nn(pick_ref[...], input_ref[...]).astype(jnp.bfloat16)
    send_grad[...] = (weight * dot_nn(pick_ref[...], grad_ref[...])).astype(jnp.bfloat16)

    def slot_span(owner):
        return aligned(owner * slots, slots, 16)

    def chunk_span(step):
        return aligned(lax.rem(chip - step + chunks, chunks) * block, block, 16)

    own = slot_span(me)
    in_columns = aligned(mine * columns, columns, 128)
    grad_columns = aligned((at_x * side_y + at_y) * columns, columns, 128)
    rows_in[own, in_columns] = send_in[own, :]
    rows_grad[own, grad_columns] = send_grad[own, :]
    pl.semaphore_wait(barrier, n_sp + n_tp - 2)

    def send_rows(owner):
        remote(
            send_in.at[slot_span(owner), :],
            rows_in.at[own, in_columns],
            in_send.at[owner],
            in_recv.at[me],
            owner,
            mine,
        ).start()
        remote(
            send_grad.at[slot_span(owner), :],
            rows_grad.at[own, grad_columns],
            grad_send.at[owner],
            grad_recv.at[me],
            owner,
            mine,
        ).start()

    def wait_rows(owner):
        remote(
            send_in.at[own, :],
            rows_in.at[slot_span(owner), in_columns],
            in_send.at[owner],
            in_recv.at[owner],
            owner,
            mine,
        ).wait_recv()
        remote(
            send_grad.at[own, :],
            rows_grad.at[slot_span(owner), grad_columns],
            grad_send.at[owner],
            grad_recv.at[owner],
            owner,
            mine,
        ).wait_recv()

    def row_x(step):
        return lax.rem(at_x + step, side_x)

    def row_y(step):
        return lax.rem(at_y + step, side_y)

    def in_first(rows, step, index):
        return remote(
            rows_in.at[rows, in_columns],
            rows_in.at[rows, in_columns],
            in1_send.at[index, step - 1],
            in1_recv.at[index, step - 1],
            me,
            at_y * side_x + row_x(step),
        )

    def in_second(rows, step, index):
        span = aligned(at_y * side_x * columns, side_x * columns, 128)
        return remote(
            rows_in.at[rows, span],
            rows_in.at[rows, span],
            in2_send.at[index, step - 1],
            in2_recv.at[index, step - 1],
            me,
            row_y(step) * side_x + at_x,
        )

    def grad_first(rows, step, index):
        return remote(
            rows_grad.at[rows, grad_columns],
            rows_grad.at[rows, grad_columns],
            grad1_send.at[index, step - 1],
            grad1_recv.at[index, step - 1],
            me,
            row_y(step) * side_x + at_x,
        )

    def grad_second(rows, step, index):
        span = aligned(at_x * side_y * columns, side_y * columns, 128)
        return remote(
            rows_grad.at[rows, span],
            rows_grad.at[rows, span],
            grad2_send.at[index, step - 1],
            grad2_recv.at[index, step - 1],
            me,
            at_y * side_x + row_x(step),
        )

    def forward_first(index):
        rows = chunk_span(index)
        for step in range(1, side_x):
            in_first(rows, step, index).start()
        for step in range(1, side_y):
            grad_first(rows, step, index).start()

    def forward_second(index):
        rows = chunk_span(index)
        for step in range(1, side_x):
            in_first(rows, step, index).wait_recv()
        for step in range(1, side_y):
            in_second(rows, step, index).start()
        for step in range(1, side_y):
            grad_first(rows, step, index).wait_recv()
        for step in range(1, side_x):
            grad_second(rows, step, index).start()

    steps = peer_steps(side_y, side_x)

    def peer(step, sign=1):
        y = lax.rem(at_y + sign * step[0] + side_y, side_y)
        return y * side_x + lax.rem(at_x + sign * step[1] + side_x, side_x)

    def source_of(index, place):
        return lax.rem(chip - index + chunks, chunks) * CORES + place

    def part_copy(rows, step, index):
        target = peer(steps[step - 1])
        return remote(
            partial_ref.at[rows, aligned(target * columns, columns, 128)],
            arrived.at[step - 1, rows, :],
            part_send.at[index, step - 1],
            part_recv.at[index, step - 1],
            me,
            target,
        )

    def back_copy(owner):
        return remote(
            returned.at[slot_span(owner), :],
            back.at[own, :],
            back_send.at[owner],
            back_recv.at[me],
            owner,
            mine,
        )

    tile = min(hidden, 256)

    def compute(index):
        rows = chunk_span(index)
        for step in range(1, side_y):
            in_second(rows, step, index).wait_recv()
        for step in range(1, side_x):
            grad_second(rows, step, index).wait_recv()
        for start in range(0, hidden, tile):
            units = slice(start, start + tile)
            gate_pre = dot_nn(rows_in[rows, :], gate_w[:, units])
            up_pre = dot_nn(rows_in[rows, :], up_w[:, units])
            hidden_grad = None
            for y in range(side_y):
                for x in range(side_x):
                    left = (x * side_y + y) * columns
                    right = (y * side_x + x) * columns
                    term = dot_nt(
                        rows_grad[rows, left : left + columns],
                        down_w[units, right : right + columns],
                    )
                    hidden_grad = term if hidden_grad is None else hidden_grad + term
            sigmoid_gate = jax.nn.sigmoid(gate_pre)
            activated = gate_pre * sigmoid_gate
            hidden_ref[rows, units] = (activated * up_pre).astype(jnp.bfloat16)
            gate_grad_ref[rows, units] = (
                hidden_grad * up_pre * sigmoid_gate * (1.0 + gate_pre * (1.0 - sigmoid_gate))
            ).astype(jnp.bfloat16)
            up_grad_ref[rows, units] = (hidden_grad * activated).astype(jnp.bfloat16)
        for place in range(n_tp):
            span = slice(place * columns, (place + 1) * columns)
            value = dot_nt(gate_grad_ref[rows, :], gate_w[span, :])
            value = value + dot_nt(up_grad_ref[rows, :], up_w[span, :])
            partial_ref[rows, span] = value.astype(jnp.bfloat16)
        for step in range(1, n_tp):
            part_copy(rows, step, index).start()

    def give_back(index):
        rows = chunk_span(index)
        value = partial_ref[rows, in_columns].astype(jnp.float32)
        for step in range(1, n_tp):
            part_copy(rows, step, index).wait_recv()
            value = value + arrived[step - 1, rows, :].astype(jnp.float32)
        returned[rows, :] = value.astype(jnp.bfloat16)
        for place in range(CORES):
            owner = source_of(index, place)

            @pl.when(owner == me)
            def _():
                back[own, :] = returned[own, :]

            @pl.when(owner != me)
            def _():
                back_copy(owner).start()

    partner = chip * CORES + (1 - core)

    def send_chunk(index):
        for place in range(CORES):
            send_rows(lax.rem(chip + index, chunks) * CORES + place)

    def wait_chunk(index):
        for place in range(CORES):
            wait_rows(source_of(index, place))

    def span_copy(step):
        return remote(
            spans.at[me],
            spans.at[me],
            span_send.at[step - 1],
            span_recv.at[step - 1],
            lax.rem(me + step, n_sp),
            mine,
        )

    send_rows(partner)
    for index in range(1, chunks):
        send_chunk(index)
    wait_rows(partner)
    forward_first(0)
    span_kernel(key_ref, value_ref, decay_ref, spans.at[me])
    for step in range(1, n_sp):
        span_copy(step).start()
    if chunks > 1:
        wait_chunk(1)
        forward_first(1)
    forward_second(0)
    for load in loads:
        load.wait()

    def step_of(turn, carry):
        @pl.when(turn < chunks)
        def _():
            wait_chunk(turn)
            forward_first(turn)

        @pl.when(turn - 1 < chunks)
        def _():
            forward_second(turn - 1)

        compute(turn - 2)

        @pl.when(turn > 2)
        def _():
            give_back(turn - 3)

        return carry

    lax.fori_loop(2, chunks + 2, step_of, 0)

    depth = min(256, rows_in.shape[1])

    def input_tile(turn, carry):
        span = aligned(turn * depth, depth, 128)
        tile_in = rows_in[:, span]
        gate_part[span, :] = dot_tn(tile_in, gate_grad_ref[...]).astype(jnp.bfloat16)
        up_part[span, :] = dot_tn(tile_in, up_grad_ref[...]).astype(jnp.bfloat16)
        return carry

    lax.fori_loop(0, rows_in.shape[1] // depth, input_tile, 0)
    stores = [
        pltpu.make_async_copy(gate_part, gate_out.at[0], local_sem.at[3]),
        pltpu.make_async_copy(up_part, up_out.at[0], local_sem.at[4]),
        pltpu.make_async_copy(down_part, down_out.at[0], local_sem.at[5]),
    ]
    stores[0].start()
    stores[1].start()
    give_back(chunks - 1)
    for y in range(side_y):
        for x in range(side_x):
            left = (x * side_y + y) * columns
            right = (y * side_x + x) * columns
            down_part[:, right : right + columns] = dot_tn(
                hidden_ref[...], rows_grad[:, left : left + columns]
            ).astype(jnp.bfloat16)
    stores[2].start()

    for step in range(1, n_sp):
        source = lax.rem(me - step + n_sp, n_sp)
        remote(
            spans.at[source],
            spans.at[source],
            span_send.at[step - 1],
            span_recv.at[step - 1],
            source,
            mine,
        ).wait_recv()
    state = jnp.zeros(state_ref.shape, jnp.float32)
    for source in range(n_sp):
        logs = jnp.sum(
            spans[source, BLOCK : BLOCK + 3, :].astype(jnp.float32), axis=0, keepdims=True
        )
        logs_ref[source : source + 1, :] = logs
        later = jnp.exp(logs) * state + spans[source, :BLOCK, :].astype(jnp.float32)
        state = jnp.where(source < me, later, state)
    state_ref[...] = state
    mixer_kernel(query_ref, key_ref, value_ref, decay_ref, state_ref, mixer_ref)

    for step in range(1, n_sp):
        source = lax.rem(me - step + n_sp, n_sp)
        remote(
            returned.at[own, :],
            back.at[slot_span(source), :],
            back_send.at[source],
            back_recv.at[source],
            source,
            mine,
        ).wait_recv()
    routed = dot_tn(pick_ref[...], back[...])
    full_ref[:, in_columns] = (grad_ref[...].astype(jnp.float32) + routed).astype(jnp.bfloat16)

    def full_copy(step):
        return remote(
            full_ref.at[:, in_columns],
            full_ref.at[:, in_columns],
            full_send.at[step - 1],
            full_recv.at[step - 1],
            me,
            peer(steps[step - 1]),
        )

    def full_arrival(step):
        source = peer(steps[step - 1], -1)
        span = aligned(source * columns, columns, 128)
        return remote(
            full_ref.at[:, span],
            full_ref.at[:, span],
            full_send.at[step - 1],
            full_recv.at[step - 1],
            me,
            source,
        )

    for step in range(1, n_tp):
        full_copy(step).start()

    share = wide // n_sp
    both = CORES * share
    groups = chunks // n_tp
    kept = aligned(core * share, share, 16)
    given = aligned((1 - core) * share, share, 16)

    def give_copy(order):
        return remote(
            product_give.at[order],
            product_got.at[order],
            give_send.at[order],
            give_recv.at[order],
            partner,
            mine,
        )

    def product_copy(order, target):
        return remote(
            product_send.at[order],
            product_in.at[chip],
            product_send_sem.at[order],
            product_recv_sem.at[chip],
            target * CORES + core,
            mine,
        )

    def product(owner, place):
        for group in range(groups):
            order = place * groups + group
            span = aligned((owner * groups + group) * both, both, 128)
            product_ref[order] = dot_tn(full_ref[:, span], mixer_ref[...])
            product_give[order] = product_ref[order, given, :].astype(jnp.bfloat16)
            give_copy(order).start()

    def product_on(owner, place):
        for group in range(groups):
            order = place * groups + group
            target = owner * groups + group
            give_copy(order).wait_recv()
            value = product_ref[order, kept, :] + product_got[order].astype(jnp.float32)

            @pl.when(target == chip)
            def _():
                project_out[...] = value

            @pl.when(target != chip)
            def _():
                product_send[order] = value.astype(jnp.bfloat16)
                product_copy(order, target).start()

    def mixer_term(owner):
        span = aligned(owner * columns, columns, 128)
        return dot_nn(full_ref[:, span], project_w[span, :])

    owners = [mine] + [peer(step, -1) for step in steps]
    load_project.wait()
    product(owners[0], 0)
    mixer_sum[...] = mixer_term(owners[0])
    for place in range(1, n_tp - 1):
        full_arrival(place).wait_recv()
        product(owners[place], place)
        mixer_sum[...] += mixer_term(owners[place])
        product_on(owners[place - 1], place - 1)
    full_arrival(n_tp - 1).wait_recv()
    mixer_grad_ref[...] = (mixer_sum[...] + mixer_term(owners[n_tp - 1])).astype(jnp.bfloat16)
    span_grad_kernel(query_ref, decay_ref, mixer_grad_ref, span_grads.at[me])

    def span_grad_copy(step):
        return remote(
            span_grads.at[me],
            span_grads.at[me],
            span_grad_send.at[step - 1],
            span_grad_recv.at[step - 1],
            lax.rem(me + step, n_sp),
            mine,
        )

    for step in range(1, n_sp):
        span_grad_copy(step).start()
    product(owners[n_tp - 1], n_tp - 1)
    product_on(owners[n_tp - 2], n_tp - 2)
    product_on(owners[n_tp - 1], n_tp - 1)
    for step in range(1, n_sp):
        source = lax.rem(me - step + n_sp, n_sp)
        remote(
            span_grads.at[source],
            span_grads.at[source],
            span_grad_send.at[step - 1],
            span_grad_recv.at[step - 1],
            source,
            mine,
        ).wait_recv()
    state_grad = jnp.zeros(state_grad_ref.shape, jnp.float32)
    for source in reversed(range(n_sp)):
        sooner = jnp.exp(logs_ref[source : source + 1, :]) * state_grad + span_grads[
            source
        ].astype(jnp.float32)
        state_grad = jnp.where(source > me, sooner, state_grad)
    state_grad_ref[...] = state_grad
    for step in range(1, chunks):
        source = lax.rem(chip - step + chunks, chunks)
        remote(
            product_send.at[0],
            product_in.at[source],
            product_send_sem.at[0],
            product_recv_sem.at[source],
            source * CORES + core,
            mine,
        ).wait_recv()
        project_out[...] += product_in[source].astype(jnp.float32)

    for step in range(1, n_tp):
        full_copy(step).wait_send()
    for step in range(1, n_sp):
        span_grad_copy(step).wait_send()
    for place in range(n_tp):
        for group in range(groups):
            order = place * groups + group
            target = owners[place] * groups + group
            give_copy(order).wait_send()

            @pl.when(target != chip)
            def _():
                product_copy(order, target).wait_send()

    for step in range(1, n_sp):
        owner = lax.rem(me + step, n_sp)
        remote(
            send_in.at[slot_span(owner), :],
            rows_in.at[own, in_columns],
            in_send.at[owner],
            in_recv.at[me],
            owner,
            mine,
        ).wait_send()
        remote(
            send_grad.at[slot_span(owner), :],
            rows_grad.at[own, grad_columns],
            grad_send.at[owner],
            grad_recv.at[me],
            owner,
            mine,
        ).wait_send()
        back_copy(owner).wait_send()
        span_copy(step).wait_send()

    def drain(index, carry):
        rows = chunk_span(index)
        for step in range(1, side_x):
            in_first(rows, step, index).wait_send()
            grad_second(rows, step, index).wait_send()
        for step in range(1, side_y):
            in_second(rows, step, index).wait_send()
            grad_first(rows, step, index).wait_send()
        for step in range(1, n_tp):
            part_copy(rows, step, index).wait_send()
        return carry

    lax.fori_loop(0, chunks, drain, 0)
    for store in stores:
        store.wait()


def expert_call(arguments, n_sp, n_tp):
    routes, weights, inputs, grads, gate, up, down, project, queries, keys, values, decay = (
        arguments
    )
    tokens, columns = inputs.shape
    wide, hidden = gate.shape[1:]
    slots = -(-(5 * tokens * TOP) // (4 * n_sp))
    slots = -(-slots // 16) * 16
    total = n_sp * slots
    chunks = n_sp // CORES
    side_y, side_x = grid_sides(n_tp)
    width = keys.shape[1]
    share = wide // n_sp
    vmem, anywhere = (
        pl.BlockSpec(memory_space=pltpu.VMEM),
        pl.BlockSpec(memory_space=pl.ANY),
    )
    dma = pltpu.SemaphoreType.DMA

    def kernel(*refs):
        expert_kernel(n_sp, n_tp, slots, *refs)

    def bf(*shape):
        return pltpu.VMEM(shape, jnp.bfloat16)

    return pl.pallas_call(
        kernel,
        out_shape=(
            jax.ShapeDtypeStruct(gate.shape, jnp.bfloat16),
            jax.ShapeDtypeStruct(up.shape, jnp.bfloat16),
            jax.ShapeDtypeStruct(down.shape, jnp.bfloat16),
            jax.ShapeDtypeStruct((wide // n_sp, columns), jnp.float32),
            jax.ShapeDtypeStruct(values.shape, jnp.bfloat16),
            jax.ShapeDtypeStruct((BLOCK, width), jnp.float32),
            jax.ShapeDtypeStruct((BLOCK, width), jnp.float32),
        ),
        in_specs=[vmem] * 4 + [anywhere] * 4 + [vmem] * 4,
        out_specs=(anywhere, anywhere, anywhere, vmem, vmem, vmem, vmem),
        scratch_shapes=[
            bf(tokens, columns),
            pltpu.VMEM((n_sp, width), jnp.float32),
            bf(wide, columns),
            bf(tokens, wide),
            pltpu.VMEM((tokens, columns), jnp.float32),
            bf(n_sp, BLOCK, width),
            pltpu.VMEM((chunks, CORES * share, columns), jnp.float32),
            bf(chunks, share, columns),
            bf(chunks, share, columns),
            bf(chunks, share, columns),
            bf(chunks, share, columns),
            bf(wide, hidden),
            bf(wide, hidden),
            bf(hidden, wide),
            bf(wide, hidden),
            bf(wide, hidden),
            bf(hidden, wide),
            bf(total, tokens),
            bf(total, columns),
            bf(total, columns),
            bf(total, wide),
            bf(total, wide),
            bf(total, hidden),
            bf(total, hidden),
            bf(total, hidden),
            bf(total, wide),
            bf(n_tp - 1, total, columns),
            bf(total, columns),
            bf(total, columns),
            bf(n_sp, BLOCK + LOG_ROWS, width),
            dma((7,)),
            dma((n_sp,)),
            dma((n_sp,)),
            dma((n_sp,)),
            dma((n_sp,)),
            dma((chunks, max(1, side_x - 1))),
            dma((chunks, max(1, side_x - 1))),
            dma((chunks, max(1, side_y - 1))),
            dma((chunks, max(1, side_y - 1))),
            dma((chunks, max(1, side_y - 1))),
            dma((chunks, max(1, side_y - 1))),
            dma((chunks, max(1, side_x - 1))),
            dma((chunks, max(1, side_x - 1))),
            dma((chunks, n_tp - 1)),
            dma((chunks, n_tp - 1)),
            dma((n_sp,)),
            dma((n_sp,)),
            dma((n_sp - 1,)),
            dma((n_sp - 1,)),
            dma((n_tp - 1,)),
            dma((n_tp - 1,)),
            dma((n_sp - 1,)),
            dma((n_sp - 1,)),
            dma((chunks,)),
            dma((chunks,)),
            dma((chunks,)),
            dma((chunks,)),
        ],
        compiler_params=pltpu.CompilerParams(
            collective_id=0, has_side_effects=True, vmem_limit_bytes=56 * 1024 * 1024
        ),
    )(*arguments)


def body(
    moe_input,
    out_grad,
    routes,
    route_weight,
    w_gate,
    w_up,
    w_down,
    w_out,
    queries,
    key_rows,
    value_rows,
    log_decay,
):
    sp_count, tp_count = (lax.axis_size("sp"), lax.axis_size("tp"))
    token_count = out_grad.shape[0]
    width, values = (key_rows.shape[1], value_rows.shape[1])
    parts = expert_call(
        (
            routes.T,
            route_weight.T,
            moe_input,
            out_grad,
            w_gate,
            w_up,
            w_down,
            w_out,
            queries,
            key_rows,
            value_rows,
            log_decay,
        ),
        sp_count,
        tp_count,
    )
    gate_part, up_part, down_part, grad_proj, mixer_grad, state_in, state_out_grad = parts
    vmem, anywhere = (
        pl.BlockSpec(memory_space=pltpu.VMEM),
        pl.BlockSpec(memory_space=pl.ANY),
    )
    moved = (gate_part, up_part, down_part, grad_proj)
    return pl.pallas_call(
        finish_kernel,
        out_shape=[jax.ShapeDtypeStruct(part.shape, part.dtype) for part in moved]
        + [
            jax.ShapeDtypeStruct(queries.shape, jnp.bfloat16),
            jax.ShapeDtypeStruct(key_rows.shape, jnp.bfloat16),
            jax.ShapeDtypeStruct(value_rows.shape, jnp.bfloat16),
            jax.ShapeDtypeStruct(log_decay.shape, jnp.float32),
        ],
        in_specs=[anywhere] * 4 + [vmem] * 7,
        out_specs=[anywhere] * 4 + [vmem] * 4,
        scratch_shapes=[pltpu.VMEM((token_count // BLOCK, values, width), jnp.float32)]
        + [pltpu.VMEM(part.shape, part.dtype) for part in moved]
        + [pltpu.SemaphoreType.DMA((2, len(moved)))],
        compiler_params=pltpu.CompilerParams(vmem_limit_bytes=32 * 1024 * 1024),
    )(*moved, queries, key_rows, value_rows, log_decay, mixer_grad, state_in, state_out_grad)


def solution(mesh):
    in_specs = (
        P("sp", "tp"),
        P("sp", "tp"),
        P("sp", None),
        P("sp", None),
        P("sp", None, "tp"),
        P("sp", None, "tp"),
        P("sp", "tp", None),
        P(None, "tp"),
        P("sp", "tp"),
        P("sp", "tp"),
        P("sp", "tp"),
        P("sp", "tp"),
    )
    out_specs = (
        P("sp", None, "tp"),
        P("sp", None, "tp"),
        P("sp", "tp", None),
        P("sp", "tp"),
        P("sp", "tp"),
        P("sp", "tp"),
        P("sp", "tp"),
        P("sp", "tp"),
    )
    return jax.shard_map(body, mesh=mesh, in_specs=in_specs, out_specs=out_specs, check_vma=False)
```
